512 devices in a mesh: fs: 64 (over z, y), tp: 8 (over x, core).
Axes of the slice: x: 4, y: 4, z: 16, core: 2. Of those that a mesh axis runs over, the one named last changes fastest.
Arguments:
- tokens: bfloat16 [32768, 2048], P('fs'), may hold values from -6 to 6
- norm_gain: float32 [2048], P('fs'), may hold values from 0.1 to 1.9
- w_gate: float32 [64, 2048, 512], P(None, 'fs', 'tp'), may hold values from -0.125 to 0.125
- w_up: float32 [64, 2048, 512], P(None, 'fs', 'tp'), may hold values from -0.125 to 0.125
- w_down: float32 [64, 2048, 512], P(None, 'fs', 'tp'), may hold values from -0.25 to 0.25
- route_expert: int32 [32768, 2], P('fs'), may hold values from 0 to 63, as said below
- group_prob: float32 [32768], P('fs'), may hold values from 0.25 to 1
- pair_logit: float32 [32768, 2], P('fs'), may hold values from -6 to 6
Outputs:
- new_gate: bfloat16 [64, 2048, 512], P('fs', None, 'tp')
- new_up: bfloat16 [64, 2048, 512], P('fs', None, 'tp')
- new_down: bfloat16 [64, 2048, 512], P('fs', None, 'tp')
- mixed: bfloat16 [32768, 2048], P('fs', 'tp')
The draws below stay inside these ranges and needn't reach their ends.
Inputs may be any that keep to these rules, and one draw needn't show every extreme that they name: `route_expert`: each row names two different experts of one group: for its group g both lie in g * 8 to g * 8 + 7, one of 8 groups. In each aligned block of 512 rows every expert is named by exactly 16 rows, half of them in each column.
All inputs are finite; a program needn't handle non-finite values.
Results may differ from the reference program's by a relative error of at most 0.014.
Values may be sent and summed in bfloat16 or wider, within the bound.
No kernel may reach another device: no remote copies, remote signals or barrier semaphores. Data moves between devices by JAX's collectives and lax.ppermute only.
A program may use at most 64 MiB of HBM per device.

```python
import jax
import jax.numpy as jnp
from jax import lax

D = 2048
FF = 512
EPG = 8
TOP = 2
ROWS = 512
EXPERTS = 64
GROUPS = 8
CAP = 16
TOKENS = 32768
N_TP = 8


def draw_route_expert(key, part):
    block_count = TOKENS // ROWS
    half_cap = CAP // 2
    per_group = EPG * half_cap

    def one_block(block_key):
        key_order, key_shift, key_label, key_group = jax.random.split(block_key, 4)
        order = jax.random.permutation(key_order, ROWS)
        position = jnp.arange(ROWS, dtype=jnp.int32)
        group_slot = position // per_group
        within = position % per_group
        first_local = within % EPG
        shifts = jax.random.randint(key_shift, (GROUPS,), 1, EPG)
        second_local = (first_local + shifts[group_slot]) % EPG
        relabel = jax.vmap(lambda label_key: jax.random.permutation(label_key, EPG))(jax.random.split(key_label, GROUPS))
        group_perm = jax.random.permutation(key_group, GROUPS)
        chosen_group = group_perm[group_slot]
        first_expert = chosen_group * EPG + relabel[group_slot, first_local]
        second_expert = chosen_group * EPG + relabel[group_slot, second_local]
        paired = jnp.stack([first_expert, second_expert], axis=1).astype(jnp.int32)
        return jnp.zeros((ROWS, TOP), jnp.int32).at[order].set(paired)
    block_keys = jax.random.split(jax.random.fold_in(key, 7), block_count)
    return jax.vmap(one_block)(block_keys).reshape(TOKENS, TOP)


def levels(own_key, extent, shards, least, top_value):
    def one(axis_at, shards_of):
        draws = jax.random.uniform(jax.random.fold_in(jax.random.fold_in(own_key, 6), axis_at), (shards_of,), jnp.float32, least / len(shards), top_value / len(shards))
        return jnp.repeat(jnp.exp(draws), extent[axis_at] // shards_of).reshape((-1,) + (1,) * (len(extent) - axis_at - 1))

    loudness = one(*shards[0])
    for cut in shards[1:]:
        loudness = loudness * one(*cut)
    return loudness


def gaussian(key, extent, deviation, reach, shards=(), kind=jnp.bfloat16):
    array = jax.random.normal(key, extent, jnp.float32) * deviation
    if len(shards) > 0:
        array = levels(key, extent, shards, -0.22, 0.18) * array
    return jnp.clip(array, min=-reach, max=reach).astype(kind)


def setup_inputs(seed: int = 0) -> dict:
    streams_of = jax.random.split(jax.random.key(seed), 9)
    tokens = gaussian(streams_of[0], (TOKENS, D), 1.0, 6.0, ((0, 64),))
    norm_gain = jnp.clip(1.0 + 0.18 * jax.random.normal(streams_of[1], (D,), jnp.float32), 0.1, 1.9)
    w_gate = gaussian(streams_of[2], (EXPERTS, D, FF), D ** -0.5, 0.125, ((1, 64), (2, 8)), jnp.float32)
    w_up = gaussian(streams_of[3], (EXPERTS, D, FF), D ** -0.5, 0.125, ((1, 64), (2, 8)), jnp.float32)
    w_down = gaussian(streams_of[4], (EXPERTS, D, FF), FF ** -0.5, 0.25, ((1, 64), (2, 8)), jnp.float32)
    route_expert = draw_route_expert(jax.random.fold_in(streams_of[8], 71), 0)
    group_prob = jnp.clip(0.25 + 0.75 * jax.random.uniform(streams_of[6], (TOKENS,), jnp.float32) ** levels(streams_of[6], (TOKENS,), ((0, 64),), -0.2, 0.2), 0.25, 1.0)
    pair_logit = gaussian(streams_of[7], (TOKENS, TOP), 1.5, 6.0, ((0, 64),), jnp.float32)
    return {"tokens": tokens, "norm_gain": norm_gain, "w_gate": w_gate, "w_up": w_up, "w_down": w_down, "route_expert": route_expert, "group_prob": group_prob, "pair_logit": pair_logit}


EPSILON = 1e-06

def reference(tokens, norm_gain, w_gate, w_up, w_down, route_expert, group_prob, pair_logit):
    row_scale = norm_gain[None, :, None]
    new_gate = (w_gate * row_scale).astype(jnp.bfloat16)
    new_up = (w_up * row_scale).astype(jnp.bfloat16)
    new_down = w_down.astype(jnp.bfloat16)
    widened = tokens.astype(jnp.float32)
    normed = (widened * lax.rsqrt(lax.optimization_barrier(jnp.mean(widened * widened, axis=1, keepdims=True)) + EPSILON)).astype(jnp.bfloat16)
    flat_ids = route_expert.reshape(-1).astype(jnp.int32)
    order = jnp.argsort(flat_ids, stable=True).astype(jnp.int32)
    per_expert = flat_ids.shape[0] // EXPERTS
    rows_of = (order // TOP).astype(jnp.int32).reshape(EXPERTS, per_expert)
    block_width = FF // N_TP

    def one_expert(operands):
        row_ids, gate_matrix, up_matrix, down_matrix = operands
        chosen = normed[row_ids]
        gate_pre = jnp.dot(chosen, gate_matrix, preferred_element_type=jnp.float32)
        up_pre = jnp.dot(chosen, up_matrix, preferred_element_type=jnp.float32)
        hidden = lax.optimization_barrier((jax.nn.silu(gate_pre) * up_pre).astype(jnp.bfloat16))
        split_hidden = hidden.astype(jnp.float32).reshape(per_expert, N_TP, block_width)
        split_down = down_matrix.astype(jnp.float32).reshape(D, N_TP, block_width)
        parts = jnp.einsum('rnk,dnk->nrd', split_hidden, split_down).astype(jnp.bfloat16)
        parts = lax.optimization_barrier(parts)
        return lax.optimization_barrier(jnp.sum(parts.astype(jnp.float32), axis=0)).astype(jnp.bfloat16)
    results = lax.map(one_expert, (rows_of, new_gate, new_up, new_down))
    per_slot = jnp.zeros((flat_ids.shape[0], D), jnp.bfloat16).at[order].set(results.reshape(-1, D))
    per_slot = lax.optimization_barrier(per_slot)
    per_slot = per_slot.reshape(TOKENS, TOP, D).astype(jnp.float32)
    logit_gap = pair_logit[:, 0] - pair_logit[:, 1]
    weight_first = group_prob * jax.nn.sigmoid(logit_gap)
    weight_second = group_prob * jax.nn.sigmoid(-logit_gap)
    mixed = (weight_first[:, None] * per_slot[:, 0] + weight_second[:, None] * per_slot[:, 1]).astype(jnp.bfloat16)
    return (new_gate, new_up, new_down, mixed)
```

```python
import jax
import jax.numpy as jnp
from jax import lax
from jax.experimental import pallas as pl
from jax.experimental.pallas import tpu as pltpu
from jax.sharding import Mesh, PartitionSpec as P

D = 2048
EPSILON = 1e-06
FS = ("g", "l", "y")
TP = ("x", "c")
IN_GROUP = ("l", "y", "x", "c")
BF = jnp.bfloat16
F32 = jnp.float32


def expert_kernel(*refs):
    x_ref, shards, out_ref, acc = refs[0], refs[1:-2], refs[-2], refs[-1]
    x = x_ref[...]
    groups = [(r,) for r in shards[:6]] + [shards[6:8], shards[8:10]]

    def gate_up(group):
        return jnp.concatenate([r[:, :32, :].reshape(-1, 128) for r in group], axis=0)

    def down(group):
        return jnp.concatenate([r[:, 32:, :].reshape(-1, 128) for r in group], axis=0)

    lane = lax.broadcasted_iota(jnp.int32, (128, 256), 1) % 128
    low = lane < 64
    for k in range(4):
        a, b = groups[2 * k], groups[2 * k + 1]
        both = jnp.concatenate([gate_up(a), gate_up(b)], axis=1)
        pre = jnp.dot(x, both, preferred_element_type=F32)
        other = jnp.concatenate(
            [pltpu.roll(pre[:, :128], 64, 1), pltpu.roll(pre[:, 128:], 64, 1)], axis=1
        )
        gate = jnp.where(low, pre, other)
        up = jnp.where(low, other, pre)
        hidden = gate / (1.0 + jnp.exp(-gate)) * up
        stacked = jnp.concatenate(
            [jnp.where(low, hidden, 0.0), jnp.where(low, 0.0, hidden)], axis=0
        ).astype(BF)
        down_pair = jnp.concatenate([down(a), down(b)], axis=1)
        part = lax.dot_general(
            stacked, down_pair, (((1,), (1,)), ((), ())), preferred_element_type=F32
        )
        if k == 0:
            acc[...] = part
        else:
            acc[...] += part
    for j in range(8):
        for t in range(8):
            for h in range(2):
                out_ref[8 * j + t, :, 128 * h : 128 * (h + 1)] = acc[
                    128 * h + 16 * j : 128 * h + 16 * (j + 1), 128 * t : 128 * (t + 1)
                ].astype(BF)


def expert(rows, shards):
    return pl.pallas_call(
        expert_kernel,
        out_shape=jax.ShapeDtypeStruct((64, 16, 256), BF),
        scratch_shapes=[pltpu.VMEM((256, 1024), F32)],
        name="expert",
    )(rows, *shards)


def gather_weights(own):
    def along_x(v, by):
        return lax.ppermute(v, "x", [(i, (i + by) % 4) for i in range(4)])

    def swap(v):
        return lax.ppermute(v, "c", [(0, 1), (1, 0)])

    left = along_x(own, 1)
    right = along_x(own, -1)
    own_c = swap(own)
    far_a = along_x(left[:32], 1)
    far_b = along_x(right[32:], -1)
    left_c, right_c = swap(left), swap(right)
    far_a_c, far_b_c = swap(far_a), swap(far_b)
    return (own, left, right, own_c, left_c, right_c, far_a, far_b, far_a_c, far_b_c)


def local(tokens, norm_gain, w_gate, w_up, w_down, route_expert, group_prob, pair_logit):
    scale = norm_gain[None, :, None]
    gate_up = jnp.concatenate([w_gate * scale, w_up * scale], axis=2).astype(BF)
    down = jnp.concatenate([w_down[:, :16], w_down[:, 16:]], axis=2).astype(BF)
    packed = jnp.concatenate([gate_up, down], axis=1)
    own = lax.all_to_all(packed, FS, split_axis=0, concat_axis=0, tiled=True)
    new_gate = own[:, :32, :64].reshape(1, D, 64)
    new_up = own[:, :32, 64:].reshape(1, D, 64)
    new_down = jnp.concatenate([own[:, 32:, :64], own[:, 32:, 64:]], axis=1).reshape(1, D, 64)

    my_share = lax.axis_index(TP)
    first, second = route_expert[:, 0], route_expert[:, 1]
    group = first // 8
    experts = jnp.arange(64, dtype=jnp.int32)
    hot_first = first[:, None] == experts[None, :]
    hot_second = second[:, None] == experts[None, :]
    named = (hot_first | hot_second).astype(BF)
    row_at = jnp.arange(512, dtype=jnp.int32)
    before = (row_at[None, :] < row_at[:, None]).astype(BF)
    earlier = jnp.dot(before, named, preferred_element_type=F32)
    rank_first = jnp.sum(jnp.where(hot_first, earlier, 0.0), axis=1).astype(jnp.int32)
    rank_second = jnp.sum(jnp.where(hot_second, earlier, 0.0), axis=1).astype(jnp.int32)
    same_group = group[:, None] == experts[None, :] // 8
    rank_group = (jnp.sum(jnp.where(same_group, earlier, 0.0), axis=1) * 0.5).astype(jnp.int32)
    slot = group * 64 + rank_group

    def send_at(e, rank):
        return jnp.where(rank // 2 == my_share, ((e % 8) * 8 + e // 8) * 2 + rank % 2, -1)

    send_rows = jnp.arange(128, dtype=jnp.int32)[:, None]
    pick = (
        (send_at(first, rank_first)[None, :] == send_rows)
        | (send_at(second, rank_second)[None, :] == send_rows)
    ).astype(BF)
    chosen = jnp.dot(pick, tokens, preferred_element_type=F32)
    normed = (
        chosen * lax.rsqrt(jnp.mean(chosen * chosen, axis=1, keepdims=True) + EPSILON)
    ).astype(BF)
    received = lax.all_to_all(
        normed.reshape(64, 32, 128), ("l", "y", "g"), split_axis=0, concat_axis=0, tiled=True
    )

    gap = pair_logit[:, 0] - pair_logit[:, 1]
    weight_first = group_prob * jax.nn.sigmoid(gap)
    weight_second = group_prob * jax.nn.sigmoid(-gap)
    high_first = lax.reduce_precision(weight_first, 8, 7)
    high_second = lax.reduce_precision(weight_second, 8, 7)
    facts = jnp.stack(
        [
            ((first % 8) * 16 + rank_first).astype(F32),
            ((second % 8) * 16 + rank_second).astype(F32),
            high_first,
            high_second,
            weight_first - high_first,
            weight_second - high_second,
            jnp.zeros_like(gap),
            jnp.zeros_like(gap),
        ]
    ).astype(BF)
    to_slot = (slot[:, None] == row_at[None, :]).astype(BF)
    facts = jnp.dot(facts, to_slot, preferred_element_type=F32).astype(BF)
    facts = facts.reshape(8, 8, 64).transpose(1, 0, 2)
    facts = lax.all_to_all(facts, "g", split_axis=0, concat_axis=0, tiled=True)
    facts = facts.transpose(1, 0, 2).reshape(8, 512).astype(F32)
    code = facts[:2].astype(jnp.int32)
    source = row_at // 64
    at = (code // 16 * 8 + code % 16 // 2) * 16 + source[None, :] * 2 + code % 2
    slots = jnp.arange(1024, dtype=jnp.int32)[:, None]
    is_first, is_second = at[0][None, :] == slots, at[1][None, :] == slots
    mix_high = jnp.where(is_first, facts[2][None, :], jnp.where(is_second, facts[3][None, :], 0.0))
    mix_low = jnp.where(is_first, facts[4][None, :], jnp.where(is_second, facts[5][None, :], 0.0))
    mix_high, mix_low = mix_high.astype(BF), mix_low.astype(BF)

    shards = gather_weights(own)
    outs = expert(received.reshape(128, D), shards)
    back = lax.all_to_all(outs, IN_GROUP, split_axis=0, concat_axis=0, tiled=True)
    back = back.reshape(1024, 256)
    over_slots = (((0,), (0,)), ((), ()))
    mixed = (
        lax.dot_general(mix_high, back, over_slots, preferred_element_type=F32)
        + lax.dot_general(mix_low, back, over_slots, preferred_element_type=F32)
    ).astype(BF)
    home = lax.all_to_all(
        mixed.reshape(8, 64, 256), "g", split_axis=0, concat_axis=0, tiled=True
    ).reshape(512, 256)
    home = jnp.dot(to_slot, home, preferred_element_type=F32).astype(BF)
    feature = jnp.arange(256, dtype=jnp.int32)
    lies_at = (feature // 16 % 2) * 128 + feature // 32 * 16 + feature % 16
    reorder = (lies_at[None, :] == feature[:, None]).astype(BF)
    home = jnp.dot(home, reorder, preferred_element_type=F32).astype(BF)
    return new_gate, new_up, new_down, home


def solution(mesh):
    fine = Mesh(mesh.devices.reshape(8, 2, 4, 4, 2), ("g", "l", "y", "x", "c"))
    placed = (
        P(FS, None),
        P(FS),
        P(None, FS, TP),
        P(None, FS, TP),
        P(None, FS, TP),
        P(FS, None),
        P(FS),
        P(FS, None),
    )
    return jax.shard_map(
        local,
        mesh=fine,
        in_specs=placed,
        out_specs=(P(FS, None, TP), P(FS, None, TP), P(FS, None, TP), P(FS, TP)),
        check_vma=False,
    )
```

```python
import jax
import jax.numpy as jnp
from jax import lax
from jax.experimental import pallas as pl
from jax.experimental.pallas import tpu as pltpu
from jax.sharding import Mesh, PartitionSpec as P

D = 2048
EPSILON = 1e-06
FS = ("g", "l", "y")
TP = ("x", "c")
IN_GROUP = ("l", "y", "x", "c")
BF = jnp.bfloat16
F32 = jnp.float32


def hidden_and_down(x, groups, acc, first):
    def gate_up(group):
        return jnp.concatenate([r[:, :32, :].reshape(-1, 128) for r in group], axis=0)

    def down(group):
        return jnp.concatenate([r[:, 32:, :].reshape(-1, 128) for r in group], axis=0)

    lane = lax.broadcasted_iota(jnp.int32, (128, 256), 1) % 128
    low = lane < 64
    for k in range(len(groups) // 2):
        a, b = groups[2 * k], groups[2 * k + 1]
        both = jnp.concatenate([gate_up(a), gate_up(b)], axis=1)
        pre = jnp.dot(x, both, preferred_element_type=F32)
        other = jnp.concatenate(
            [pltpu.roll(pre[:, :128], 64, 1), pltpu.roll(pre[:, 128:], 64, 1)], axis=1
        )
        gate = jnp.where(low, pre, other)
        up = jnp.where(low, other, pre)
        hidden = gate / (1.0 + jnp.exp(-gate)) * up
        stacked = jnp.concatenate(
            [jnp.where(low, hidden, 0.0), jnp.where(low, 0.0, hidden)], axis=0
        ).astype(BF)
        down_pair = jnp.concatenate([down(a), down(b)], axis=1)
        part = lax.dot_general(
            stacked, down_pair, (((1,), (1,)), ((), ())), preferred_element_type=F32
        )
        if k == 0 and first:
            acc[...] = part
        else:
            acc[...] += part


def near_kernel(x_ref, *refs):
    shards, acc = refs[:-1], refs[-1]
    halves = [shards[2 * i : 2 * i + 2] for i in range(6)]
    hidden_and_down(x_ref[...], halves, acc, True)


def far_kernel(x_ref, near_ref, *refs):
    shards, out_ref, acc = refs[:4], refs[4], refs[5]
    acc[...] = near_ref[...]
    hidden_and_down(x_ref[...], [shards[:2], shards[2:]], acc, False)
    for j in range(8):
        for t in range(8):
            for h in range(2):
                out_ref[8 * j + t, :, 128 * h : 128 * (h + 1)] = acc[
                    128 * h + 16 * j : 128 * h + 16 * (j + 1), 128 * t : 128 * (t + 1)
                ].astype(BF)


def expert(rows, near, far):
    partial = pl.pallas_call(
        near_kernel,
        out_shape=jax.ShapeDtypeStruct((256, 1024), F32),
        name="expert_near",
    )(rows, *near)
    return pl.pallas_call(
        far_kernel,
        out_shape=jax.ShapeDtypeStruct((64, 16, 256), BF),
        scratch_shapes=[pltpu.VMEM((256, 1024), F32)],
        name="expert_far",
    )(rows, partial, *far)


def gather_weights(own):
    def along_x(v, by):
        return lax.ppermute(v, "x", [(i, (i + by) % 4) for i in range(4)])

    def swap(v):
        return lax.ppermute(v, "c", [(0, 1), (1, 0)])

    own = [own[:32], own[32:]]
    left_a, right_b = along_x(own[0], 1), along_x(own[1], -1)
    left_b, right_a = along_x(own[1], 1), along_x(own[0], -1)
    far = [along_x(left_a, 1), along_x(right_b, -1)]
    near = own + [left_a, left_b, right_a, right_b]
    return near + [swap(v) for v in near], far + [swap(v) for v in far]


def local(tokens, norm_gain, w_gate, w_up, w_down, route_expert, group_prob, pair_logit):
    scale = norm_gain[None, :, None]
    gate_up = jnp.concatenate([w_gate * scale, w_up * scale], axis=2).astype(BF)
    down = jnp.concatenate([w_down[:, :16], w_down[:, 16:]], axis=2).astype(BF)
    packed = jnp.concatenate([gate_up, down], axis=1)
    own = lax.all_to_all(packed, FS, split_axis=0, concat_axis=0, tiled=True)
    new_gate = own[:, :32, :64].reshape(1, D, 64)
    new_up = own[:, :32, 64:].reshape(1, D, 64)
    new_down = jnp.concatenate([own[:, 32:, :64], own[:, 32:, 64:]], axis=1).reshape(1, D, 64)

    my_share = lax.axis_index(TP)
    first, second = route_expert[:, 0], route_expert[:, 1]
    group = first // 8
    experts = jnp.arange(64, dtype=jnp.int32)
    hot_first = first[:, None] == experts[None, :]
    hot_second = second[:, None] == experts[None, :]
    named = (hot_first | hot_second).astype(BF)
    row_at = jnp.arange(512, dtype=jnp.int32)
    before = (row_at[None, :] < row_at[:, None]).astype(BF)
    earlier = jnp.dot(before, named, preferred_element_type=F32)
    rank_first = jnp.sum(jnp.where(hot_first, earlier, 0.0), axis=1).astype(jnp.int32)
    rank_second = jnp.sum(jnp.where(hot_second, earlier, 0.0), axis=1).astype(jnp.int32)
    same_group = group[:, None] == experts[None, :] // 8
    rank_group = (jnp.sum(jnp.where(same_group, earlier, 0.0), axis=1) * 0.5).astype(jnp.int32)
    slot = group * 64 + rank_group

    def send_at(e, rank):
        return jnp.where(rank // 2 == my_share, ((e % 8) * 8 + e // 8) * 2 + rank % 2, -1)

    send_rows = jnp.arange(128, dtype=jnp.int32)[:, None]
    pick = (
        (send_at(first, rank_first)[None, :] == send_rows)
        | (send_at(second, rank_second)[None, :] == send_rows)
    ).astype(BF)
    chosen = jnp.dot(pick, tokens, preferred_element_type=F32)
    normed = (
        chosen * lax.rsqrt(jnp.mean(chosen * chosen, axis=1, keepdims=True) + EPSILON)
    ).astype(BF)

    gap = pair_logit[:, 0] - pair_logit[:, 1]
    weight_first = group_prob * jax.nn.sigmoid(gap)
    weight_second = group_prob * jax.nn.sigmoid(-gap)
    high_first = lax.reduce_precision(weight_first, 8, 7)
    high_second = lax.reduce_precision(weight_second, 8, 7)
    facts = jnp.stack(
        [
            ((first % 8) * 16 + rank_first).astype(F32),
            ((second % 8) * 16 + rank_second).astype(F32),
            high_first,
            high_second,
            weight_first - high_first,
            weight_second - high_second,
            jnp.zeros_like(gap),
            jnp.zeros_like(gap),
        ]
    ).astype(BF)
    to_slot = (slot[:, None] == row_at[None, :]).astype(BF)
    facts = jnp.dot(facts, to_slot, preferred_element_type=F32).astype(BF)
    facts = lax.all_gather(facts.reshape(8, 8, 64).transpose(1, 0, 2), "g")
    facts = lax.dynamic_index_in_dim(facts, lax.axis_index("g"), 1, keepdims=False)
    normed, facts = lax.optimization_barrier((normed, facts))
    received = lax.all_to_all(
        normed.reshape(64, 32, 128), ("l", "y", "g"), split_axis=0, concat_axis=0, tiled=True
    )
    facts = facts.transpose(1, 0, 2).reshape(8, 512).astype(F32)
    code = facts[:2].astype(jnp.int32)
    source = row_at // 64
    at = (code // 16 * 8 + code % 16 // 2) * 16 + source[None, :] * 2 + code % 2
    slots = jnp.arange(1024, dtype=jnp.int32)[:, None]
    is_first, is_second = at[0][None, :] == slots, at[1][None, :] == slots
    mix_high = jnp.where(is_first, facts[2][None, :], jnp.where(is_second, facts[3][None, :], 0.0))
    mix_low = jnp.where(is_first, facts[4][None, :], jnp.where(is_second, facts[5][None, :], 0.0))
    mix_high, mix_low = mix_high.astype(BF), mix_low.astype(BF)

    near, far = gather_weights(own)
    outs = expert(received.reshape(128, D), near, far)
    back = lax.all_to_all(outs, IN_GROUP, split_axis=0, concat_axis=0, tiled=True)
    back = back.reshape(1024, 256)
    over_slots = (((0,), (0,)), ((), ()))
    mixed = (
        lax.dot_general(mix_high, back, over_slots, preferred_element_type=F32)
        + lax.dot_general(mix_low, back, over_slots, preferred_element_type=F32)
    ).astype(BF)
    home = lax.all_to_all(
        mixed.reshape(8, 64, 256), "g", split_axis=0, concat_axis=0, tiled=True
    ).reshape(512, 256)
    home = jnp.dot(to_slot, home, preferred_element_type=F32).astype(BF)
    feature = jnp.arange(256, dtype=jnp.int32)
    lies_at = (feature // 16 % 2) * 128 + feature // 32 * 16 + feature % 16
    reorder = (lies_at[None, :] == feature[:, None]).astype(BF)
    home = jnp.dot(home, reorder, preferred_element_type=F32).astype(BF)
    return new_gate, new_up, new_down, home


def solution(mesh):
    fine = Mesh(mesh.devices.reshape(8, 2, 4, 4, 2), ("g", "l", "y", "x", "c"))
    placed = (
        P(FS, None),
        P(FS),
        P(None, FS, TP),
        P(None, FS, TP),
        P(None, FS, TP),
        P(FS, None),
        P(FS),
        P(FS, None),
    )
    return jax.shard_map(
        local,
        mesh=fine,
        in_specs=placed,
        out_specs=(P(FS, None, TP), P(FS, None, TP), P(FS, None, TP), P(FS, TP)),
        check_vma=False,
    )
```

```python
import jax
import jax.numpy as jnp
from jax import lax
from jax.experimental import pallas as pl
from jax.experimental.pallas import tpu as pltpu
from jax.sharding import Mesh, PartitionSpec as P

D = 2048
EPSILON = 1e-06
FS = ("g", "l", "y")
TP = ("x", "c")
IN_GROUP = ("l", "y", "x", "c")
BF = jnp.bfloat16
F32 = jnp.float32


def expert_kernel(x_ref, *refs):
    shards, out_ref, acc = refs[:8], refs[8], refs[9]
    x = x_ref[...]
    lane = lax.broadcasted_iota(jnp.int32, (128, 256), 1) % 128
    low = lane < 64
    pieces = []
    for k in range(4):
        pair = shards[2 * k : 2 * k + 2]
        both = jnp.concatenate([r[:, :32, :].reshape(-1, 128) for r in pair], axis=1)
        pre = jnp.dot(x, both, preferred_element_type=F32)
        other = jnp.concatenate(
            [pltpu.roll(pre[:, :128], 64, 1), pltpu.roll(pre[:, 128:], 64, 1)], axis=1
        )
        gate = jnp.where(low, pre, other)
        up = jnp.where(low, other, pre)
        hidden = gate / (1.0 + jnp.exp(-gate)) * up
        pieces.append(
            jnp.concatenate(
                [jnp.where(low, hidden, 0.0), jnp.where(low, 0.0, hidden)], axis=0
            ).astype(BF)
        )
    down = jnp.concatenate([r[:, 32:, :].reshape(-1, 128) for r in shards], axis=1)
    acc[...] = lax.dot_general(
        jnp.concatenate(pieces, axis=1),
        down,
        (((1,), (1,)), ((), ())),
        preferred_element_type=F32,
    )
    for j in range(8):
        for t in range(8):
            for h in range(2):
                out_ref[8 * j + t, :, 128 * h : 128 * (h + 1)] = acc[
                    128 * h + 16 * j : 128 * h + 16 * (j + 1), 128 * t : 128 * (t + 1)
                ].astype(BF)


def expert(rows, shards):
    return pl.pallas_call(
        expert_kernel,
        out_shape=jax.ShapeDtypeStruct((64, 16, 256), BF),
        scratch_shapes=[pltpu.VMEM((256, 1024), F32)],
        name="expert",
    )(rows, *shards)


def gather_weights(own):
    around = []
    for i in range(4):
        around.append((2 * i, 2 * ((i + 1) % 4)))
        around.append((2 * i + 1, 2 * ((i + 3) % 4) + 1))

    def pass_on(v):
        return lax.ppermute(v, TP, around)

    def swap(v):
        return lax.ppermute(v, "c", [(0, 1), (1, 0)])

    near = pass_on(own)
    own_c = swap(own)
    other = pass_on(own_c)
    far = pass_on(near)
    near_c, other_c, far_c = swap(near), swap(other), swap(far)
    return own, own_c, near, near_c, other, other_c, far, far_c


def trade_facts(facts, shifts):
    mine = lax.axis_index("g")
    got = {}
    for k in shifts:
        part = lax.dynamic_index_in_dim(facts, (mine + k) & 7, 0, keepdims=False)
        if k:
            part = lax.ppermute(part, "g", [(i, (i + k) % 8) for i in range(8)])
        got[k] = part
    return got


def local(tokens, norm_gain, w_gate, w_up, w_down, route_expert, group_prob, pair_logit):
    scale = norm_gain[None, :, None]
    gate_up = jnp.concatenate([w_gate * scale, w_up * scale], axis=2).astype(BF)
    down = jnp.concatenate([w_down[:, :16], w_down[:, 16:]], axis=2).astype(BF)
    packed = jnp.concatenate([gate_up, down], axis=1)
    own = lax.all_to_all(packed, FS, split_axis=0, concat_axis=0, tiled=True)
    new_gate = own[:, :32, :64].reshape(1, D, 64)
    new_up = own[:, :32, 64:].reshape(1, D, 64)
    new_down = jnp.concatenate([own[:, 32:, :64], own[:, 32:, 64:]], axis=1).reshape(1, D, 64)

    my_share = lax.axis_index(TP)
    first, second = route_expert[:, 0], route_expert[:, 1]
    group = first // 8
    experts = jnp.arange(64, dtype=jnp.int32)
    hot_first = first[:, None] == experts[None, :]
    hot_second = second[:, None] == experts[None, :]
    named = (hot_first | hot_second).astype(BF)
    row_at = jnp.arange(512, dtype=jnp.int32)
    before = (row_at[None, :] < row_at[:, None]).astype(BF)
    earlier = jnp.dot(before, named, preferred_element_type=F32)
    rank_first = jnp.sum(jnp.where(hot_first, earlier, 0.0), axis=1).astype(jnp.int32)
    rank_second = jnp.sum(jnp.where(hot_second, earlier, 0.0), axis=1).astype(jnp.int32)
    same_group = group[:, None] == experts[None, :] // 8
    rank_group = (jnp.sum(jnp.where(same_group, earlier, 0.0), axis=1) * 0.5).astype(jnp.int32)
    slot = group * 64 + rank_group

    def send_at(e, rank):
        return jnp.where(rank // 2 == my_share, ((e % 8) * 8 + e // 8) * 2 + rank % 2, -1)

    send_rows = jnp.arange(128, dtype=jnp.int32)[:, None]
    pick = (
        (send_at(first, rank_first)[None, :] == send_rows)
        | (send_at(second, rank_second)[None, :] == send_rows)
    ).astype(BF)
    chosen = jnp.dot(pick, tokens, preferred_element_type=F32)
    mean = jnp.mean(chosen * chosen, axis=1, keepdims=True)
    normed = (chosen * lax.rsqrt(mean + EPSILON)).astype(BF).reshape(64, 32, 128)

    gap = pair_logit[:, 0] - pair_logit[:, 1]
    weight_first = group_prob * jax.nn.sigmoid(gap)
    weight_second = group_prob * jax.nn.sigmoid(-gap)
    high_first = lax.reduce_precision(weight_first, 8, 7)
    high_second = lax.reduce_precision(weight_second, 8, 7)
    facts = jnp.stack(
        [
            ((first % 8) * 16 + rank_first).astype(F32),
            ((second % 8) * 16 + rank_second).astype(F32),
            high_first,
            high_second,
            weight_first - high_first,
            weight_second - high_second,
            jnp.zeros_like(gap),
            jnp.zeros_like(gap),
        ]
    ).astype(BF)
    to_slot = (slot[:, None] == row_at[None, :]).astype(BF)
    facts = jnp.dot(facts, to_slot, preferred_element_type=F32).astype(BF)
    facts = facts.reshape(8, 8, 64).transpose(1, 0, 2)
    got = trade_facts(facts, range(2, 7))
    sent, got = lax.optimization_barrier((normed, got))
    got.update(trade_facts(facts, (0, 1, 7)))
    received = lax.all_to_all(
        sent, ("l", "y", "g"), split_axis=0, concat_axis=0, tiled=True
    )
    eight = jnp.arange(8, dtype=jnp.int32)
    from_group = ((lax.axis_index("g") - eight[:, None]) & 7 == eight[None, :]).astype(BF)
    facts = jnp.einsum("gk,kfr->fgr", from_group, jnp.stack([got[k] for k in range(8)]), preferred_element_type=F32)
    facts = facts.reshape(8, 512)
    code = facts[:2].astype(jnp.int32)
    source = row_at // 64
    at = (code // 16 * 8 + code % 16 // 2) * 16 + source[None, :] * 2 + code % 2
    slots = jnp.arange(1024, dtype=jnp.int32)[:, None]
    is_first, is_second = at[0][None, :] == slots, at[1][None, :] == slots
    mix_high = jnp.where(is_first, facts[2][None, :], jnp.where(is_second, facts[3][None, :], 0.0))
    mix_low = jnp.where(is_first, facts[4][None, :], jnp.where(is_second, facts[5][None, :], 0.0))
    mix_high, mix_low = mix_high.astype(BF), mix_low.astype(BF)
    feature = jnp.arange(256, dtype=jnp.int32)
    lies_at = (feature // 16 % 2) * 128 + feature // 32 * 16 + feature % 16
    reorder = (lies_at[None, :] == feature[:, None]).astype(BF)

    outs = expert(received.reshape(128, D), gather_weights(own))
    back = lax.all_to_all(outs, IN_GROUP, split_axis=0, concat_axis=0, tiled=True)
    back = back.reshape(1024, 256)
    over_slots = (((0,), (0,)), ((), ()))
    mixed = (
        lax.dot_general(mix_high, back, over_slots, preferred_element_type=F32)
        + lax.dot_general(mix_low, back, over_slots, preferred_element_type=F32)
    ).astype(BF)
    home = lax.all_to_all(
        mixed.reshape(8, 64, 256), "g", split_axis=0, concat_axis=0, tiled=True
    ).reshape(512, 256)
    home = jnp.dot(to_slot, home, preferred_element_type=F32).astype(BF)
    home = jnp.dot(home, reorder, preferred_element_type=F32).astype(BF)
    return new_gate, new_up, new_down, home


def solution(mesh):
    fine = Mesh(mesh.devices.reshape(8, 2, 4, 4, 2), ("g", "l", "y", "x", "c"))
    placed = (
        P(FS, None),
        P(FS),
        P(None, FS, TP),
        P(None, FS, TP),
        P(None, FS, TP),
        P(FS, None),
        P(FS),
        P(FS, None),
    )
    return jax.shard_map(
        local,
        mesh=fine,
        in_specs=placed,
        out_specs=(P(FS, None, TP), P(FS, None, TP), P(FS, None, TP), P(FS, TP)),
        check_vma=False,
    )
```

```python
import jax
import jax.numpy as jnp
from jax import lax
from jax.experimental import pallas as pl
from jax.experimental.pallas import tpu as pltpu
from jax.sharding import Mesh, PartitionSpec as P

D = 2048
EPSILON = 1e-06
FS = ("g", "l", "y")
TP = ("x", "c")
IN_GROUP = ("l", "y", "x", "c")
BF = jnp.bfloat16
F32 = jnp.float32


def pack_kernel(gain_ref, gate_ref, up_ref, down_ref, out_ref):
    along = jnp.broadcast_to(gain_ref[...], (32, 32))
    diagonal = lax.broadcasted_iota(jnp.int32, (32, 32), 0) == lax.broadcasted_iota(
        jnp.int32, (32, 32), 1
    )
    gain = jnp.sum(jnp.where(diagonal, along, 0.0), axis=1, keepdims=True)[None]
    out_ref[:, :32, :64] = (gate_ref[...] * gain).astype(BF)
    out_ref[:, :32, 64:] = (up_ref[...] * gain).astype(BF)
    out_ref[:, 32:, :64] = down_ref[:, :16, :].astype(BF)
    out_ref[:, 32:, 64:] = down_ref[:, 16:, :].astype(BF)


def pack(norm_gain, w_gate, w_up, w_down):
    return pl.pallas_call(
        pack_kernel, out_shape=jax.ShapeDtypeStruct((64, 48, 128), BF), name="pack"
    )(norm_gain.reshape(1, 32), w_gate, w_up, w_down)


def home_kernel(slot_ref, back_ref, out_ref):
    row = lax.broadcasted_iota(jnp.int32, (512, 512), 0)
    at_slot = (row == slot_ref[...]).astype(F32).astype(BF)
    rows = lax.dot_general(
        at_slot, back_ref[...], (((0,), (0,)), ((), ())), preferred_element_type=F32
    ).astype(BF)
    lies = lax.broadcasted_iota(jnp.int32, (256, 256), 0)
    feature = lax.broadcasted_iota(jnp.int32, (256, 256), 1)
    lies_at = ((feature >> 4) & 1) * 128 + (feature >> 5) * 16 + (feature & 15)
    reorder = (lies == lies_at).astype(F32).astype(BF)
    out_ref[...] = jnp.dot(rows, reorder, preferred_element_type=F32).astype(BF)


def expert_kernel(x_ref, *refs):
    shards, out_ref, acc = refs[:8], refs[8], refs[9]
    x = x_ref[...]
    lane = lax.broadcasted_iota(jnp.int32, (128, 256), 1) % 128
    low = lane < 64
    pieces = []
    for k in range(4):
        pair = shards[2 * k : 2 * k + 2]
        both = jnp.concatenate([r[:, :32, :].reshape(-1, 128) for r in pair], axis=1)
        pre = jnp.dot(x, both, preferred_element_type=F32)
        other = jnp.concatenate(
            [pltpu.roll(pre[:, :128], 64, 1), pltpu.roll(pre[:, 128:], 64, 1)], axis=1
        )
        gate = jnp.where(low, pre, other)
        up = jnp.where(low, other, pre)
        hidden = gate / (1.0 + jnp.exp(-gate)) * up
        pieces.append(
            jnp.concatenate(
                [jnp.where(low, hidden, 0.0), jnp.where(low, 0.0, hidden)], axis=0
            ).astype(BF)
        )
    down = jnp.concatenate([r[:, 32:, :].reshape(-1, 128) for r in shards], axis=1)
    acc[...] = lax.dot_general(
        jnp.concatenate(pieces, axis=1),
        down,
        (((1,), (1,)), ((), ())),
        preferred_element_type=F32,
    )
    for j in range(8):
        for t in range(8):
            for h in range(2):
                out_ref[8 * j + t, :, 128 * h : 128 * (h + 1)] = acc[
                    128 * h + 16 * j : 128 * h + 16 * (j + 1), 128 * t : 128 * (t + 1)
                ].astype(BF)


def expert(rows, shards):
    return pl.pallas_call(
        expert_kernel,
        out_shape=jax.ShapeDtypeStruct((64, 16, 256), BF),
        scratch_shapes=[pltpu.VMEM((256, 1024), F32)],
        name="expert",
    )(rows, *shards)


def gather_weights(own):
    around = []
    for i in range(4):
        around.append((2 * i, 2 * ((i + 1) % 4)))
        around.append((2 * i + 1, 2 * ((i + 3) % 4) + 1))

    def pass_on(v):
        return lax.ppermute(v, TP, around)

    def swap(v):
        return lax.ppermute(v, "c", [(0, 1), (1, 0)])

    near = pass_on(own)
    own_c = swap(own)
    other = pass_on(own_c)
    far = pass_on(near)
    near_c, other_c, far_c = swap(near), swap(other), swap(far)
    return own, own_c, near, near_c, other, other_c, far, far_c


def trade_facts(facts, shifts):
    mine = lax.axis_index("g")
    got = {}
    for k in shifts:
        part = lax.dynamic_index_in_dim(facts, (mine + k) & 7, 0, keepdims=False)
        if k:
            part = lax.ppermute(part, "g", [(i, (i + k) % 8) for i in range(8)])
        got[k] = part
    return got


def local(tokens, norm_gain, w_gate, w_up, w_down, route_expert, group_prob, pair_logit):
    packed = pack(norm_gain, w_gate, w_up, w_down)
    own = lax.all_to_all(packed, FS, split_axis=0, concat_axis=0, tiled=True)
    new_gate = own[:, :32, :64].reshape(1, D, 64)
    new_up = own[:, :32, 64:].reshape(1, D, 64)
    new_down = jnp.concatenate([own[:, 32:, :64], own[:, 32:, 64:]], axis=1).reshape(1, D, 64)

    my_share = lax.axis_index(TP)
    first, second = route_expert[:, 0], route_expert[:, 1]
    group = first // 8
    experts = jnp.arange(64, dtype=jnp.int32)
    hot_first = first[:, None] == experts[None, :]
    hot_second = second[:, None] == experts[None, :]
    named = (hot_first | hot_second).astype(BF)
    row_at = jnp.arange(512, dtype=jnp.int32)
    before = (row_at[None, :] < row_at[:, None]).astype(BF)
    earlier = jnp.dot(before, named, preferred_element_type=F32)
    rank_first = jnp.sum(jnp.where(hot_first, earlier, 0.0), axis=1).astype(jnp.int32)
    rank_second = jnp.sum(jnp.where(hot_second, earlier, 0.0), axis=1).astype(jnp.int32)
    same_group = group[:, None] == experts[None, :] // 8
    rank_group = (jnp.sum(jnp.where(same_group, earlier, 0.0), axis=1) * 0.5).astype(jnp.int32)
    slot = group * 64 + rank_group

    def send_at(e, rank):
        return jnp.where(rank // 2 == my_share, ((e % 8) * 8 + e // 8) * 2 + rank % 2, -1)

    send_rows = jnp.arange(128, dtype=jnp.int32)[:, None]
    pick = (
        (send_at(first, rank_first)[None, :] == send_rows)
        | (send_at(second, rank_second)[None, :] == send_rows)
    ).astype(BF)
    chosen = jnp.dot(pick, tokens, preferred_element_type=F32)
    mean = jnp.mean(chosen * chosen, axis=1, keepdims=True)
    normed = (chosen * lax.rsqrt(mean + EPSILON)).astype(BF).reshape(64, 32, 128)

    gap = pair_logit[:, 0] - pair_logit[:, 1]
    weight_first = group_prob * jax.nn.sigmoid(gap)
    weight_second = group_prob * jax.nn.sigmoid(-gap)
    facts = jnp.stack(
        [
            ((first % 8) * 16 + rank_first).astype(F32),
            ((second % 8) * 16 + rank_second).astype(F32),
            weight_first,
            weight_second,
            jnp.zeros_like(gap),
            jnp.zeros_like(gap),
            jnp.zeros_like(gap),
            jnp.zeros_like(gap),
        ]
    ).astype(BF)
    to_slot = (slot[:, None] == row_at[None, :]).astype(BF)
    facts = jnp.dot(facts, to_slot, preferred_element_type=F32).astype(BF)
    facts = facts.reshape(8, 8, 64).transpose(1, 0, 2)
    got = trade_facts(facts, range(1, 7))
    sent, got = lax.optimization_barrier((normed, got))
    got.update(trade_facts(facts, (0, 7)))
    received = lax.all_to_all(
        sent, ("l", "y", "g"), split_axis=0, concat_axis=0, tiled=True
    )
    eight = jnp.arange(8, dtype=jnp.int32)
    from_group = ((lax.axis_index("g") - eight[:, None]) & 7 == eight[None, :]).astype(BF)
    facts = jnp.einsum("gk,kfr->fgr", from_group, jnp.stack([got[k] for k in range(8)]), preferred_element_type=F32)
    facts = facts.reshape(8, 512)
    code = facts[:2].astype(jnp.int32)
    source = row_at // 64
    at = (code // 16 * 8 + code % 16 // 2) * 16 + source[None, :] * 2 + code % 2
    slots = jnp.arange(1024, dtype=jnp.int32)[:, None]
    is_first, is_second = at[0][None, :] == slots, at[1][None, :] == slots
    mix = jnp.where(is_first, facts[2][None, :], jnp.where(is_second, facts[3][None, :], 0.0))
    mix = mix.astype(BF)
    outs = expert(received.reshape(128, D), gather_weights(own))
    back = lax.all_to_all(outs, IN_GROUP, split_axis=0, concat_axis=0, tiled=True)
    back = back.reshape(1024, 256)
    over_slots = (((0,), (0,)), ((), ()))
    mixed = lax.dot_general(mix, back, over_slots, preferred_element_type=F32).astype(BF)
    home = lax.all_to_all(
        mixed.reshape(8, 64, 256), "g", split_axis=0, concat_axis=0, tiled=True
    ).reshape(512, 256)
    home = pl.pallas_call(
        home_kernel, out_shape=jax.ShapeDtypeStruct((512, 256), BF), name="home"
    )(slot.reshape(1, 512), home)
    return new_gate, new_up, new_down, home


def solution(mesh):
    fine = Mesh(mesh.devices.reshape(8, 2, 4, 4, 2), ("g", "l", "y", "x", "c"))
    placed = (
        P(FS, None),
        P(FS),
        P(None, FS, TP),
        P(None, FS, TP),
        P(None, FS, TP),
        P(FS, None),
        P(FS),
        P(FS, None),
    )
    return jax.shard_map(
        local,
        mesh=fine,
        in_specs=placed,
        out_specs=(P(FS, None, TP), P(FS, None, TP), P(FS, None, TP), P(FS, TP)),
        check_vma=False,
    )
```

```python
import jax
import jax.numpy as jnp
from jax import lax
from jax.experimental import pallas as pl
from jax.experimental.pallas import tpu as pltpu
from jax.sharding import Mesh, PartitionSpec as P

D = 2048
EPSILON = 1e-06
FS = ("g", "l", "y")
TP = ("x", "c")
IN_GROUP = ("l", "y", "x", "c")
BF = jnp.bfloat16
F32 = jnp.float32


HELD = (0, 6, 8)


def pack_kernel(gain_ref, gate_ref, up_ref, down_ref, out_ref):
    along = jnp.broadcast_to(gain_ref[...], (32, 32))
    diagonal = lax.broadcasted_iota(jnp.int32, (32, 32), 0) == lax.broadcasted_iota(
        jnp.int32, (32, 32), 1
    )
    gain = jnp.sum(jnp.where(diagonal, along, 0.0), axis=1, keepdims=True)[None]
    out_ref[:, :32, :64] = (gate_ref[...] * gain).astype(BF)
    out_ref[:, :32, 64:] = (up_ref[...] * gain).astype(BF)
    out_ref[:, 32:, :64] = down_ref[:, :16, :].astype(BF)
    out_ref[:, 32:, 64:] = down_ref[:, 16:, :].astype(BF)


def pack(norm_gain, w_gate, w_up, w_down):
    return pl.pallas_call(
        pack_kernel, out_shape=jax.ShapeDtypeStruct((64, 48, 128), BF), name="pack"
    )(norm_gain.reshape(1, 32), w_gate, w_up, w_down)


def home_kernel(slot_ref, back_ref, out_ref):
    row = lax.broadcasted_iota(jnp.int32, (512, 512), 0)
    at_slot = (row == slot_ref[...]).astype(F32).astype(BF)
    rows = lax.dot_general(
        at_slot, back_ref[...], (((0,), (0,)), ((), ())), preferred_element_type=F32
    ).astype(BF)
    lies = lax.broadcasted_iota(jnp.int32, (256, 256), 0)
    feature = lax.broadcasted_iota(jnp.int32, (256, 256), 1)
    lies_at = ((feature >> 4) & 1) * 128 + (feature >> 5) * 16 + (feature & 15)
    reorder = (lies == lies_at).astype(F32).astype(BF)
    out_ref[...] = jnp.dot(rows, reorder, preferred_element_type=F32).astype(BF)


def expert_kernel(x_ref, *refs):
    shards, out_ref, acc = refs[:8], refs[8], refs[9]
    x = x_ref[...]
    lane = lax.broadcasted_iota(jnp.int32, (128, 256), 1) % 128
    low = lane < 64
    pieces = []
    for k in range(4):
        pair = shards[2 * k : 2 * k + 2]
        both = jnp.concatenate([r[:, :32, :].reshape(-1, 128) for r in pair], axis=1)
        pre = jnp.dot(x, both, preferred_element_type=F32)
        other = jnp.concatenate(
            [pltpu.roll(pre[:, :128], 64, 1), pltpu.roll(pre[:, 128:], 64, 1)], axis=1
        )
        gate = jnp.where(low, pre, other)
        up = jnp.where(low, other, pre)
        hidden = gate / (1.0 + jnp.exp(-gate)) * up
        pieces.append(
            jnp.concatenate(
                [jnp.where(low, hidden, 0.0), jnp.where(low, 0.0, hidden)], axis=0
            ).astype(BF)
        )
    down = jnp.concatenate([r[:, 32:, :].reshape(-1, 128) for r in shards], axis=1)
    acc[...] = lax.dot_general(
        jnp.concatenate(pieces, axis=1),
        down,
        (((1,), (1,)), ((), ())),
        preferred_element_type=F32,
    )
    for j in range(8):
        for t in range(8):
            for h in range(2):
                out_ref[8 * j + t, :, 128 * h : 128 * (h + 1)] = acc[
                    128 * h + 16 * j : 128 * h + 16 * (j + 1), 128 * t : 128 * (t + 1)
                ].astype(BF)


def expert(rows, shards):
    operands = [rows, *shards]
    for i in HELD:
        operands[i] = pltpu.with_memory_space_constraint(operands[i], pltpu.VMEM)
    return pl.pallas_call(
        expert_kernel,
        out_shape=jax.ShapeDtypeStruct((64, 16, 256), BF),
        scratch_shapes=[pltpu.VMEM((256, 1024), F32)],
        name="expert",
    )(*operands)


def gather_weights(own):
    around = []
    for i in range(4):
        around.append((2 * i, 2 * ((i + 1) % 4)))
        around.append((2 * i + 1, 2 * ((i + 3) % 4) + 1))

    def pass_on(v):
        return lax.ppermute(v, TP, around)

    def swap(v):
        return lax.ppermute(v, "c", [(0, 1), (1, 0)])

    near = pass_on(own)
    own_c = swap(own)
    other = pass_on(own_c)
    far = pass_on(near)
    near_c, other_c, far_c = swap(near), swap(other), swap(far)
    return own, own_c, near, near_c, other, other_c, far, far_c


def trade_facts(facts, shifts):
    mine = lax.axis_index("g")
    got = {}
    for k in shifts:
        part = lax.dynamic_index_in_dim(facts, (mine + k) & 7, 0, keepdims=False)
        if k:
            part = lax.ppermute(part, "g", [(i, (i + k) % 8) for i in range(8)])
        got[k] = part
    return got


def local(tokens, norm_gain, w_gate, w_up, w_down, route_expert, group_prob, pair_logit):
    packed = pack(norm_gain, w_gate, w_up, w_down)
    own = lax.all_to_all(packed, FS, split_axis=0, concat_axis=0, tiled=True)
    new_gate = own[:, :32, :64].reshape(1, D, 64)
    new_up = own[:, :32, 64:].reshape(1, D, 64)
    new_down = jnp.concatenate([own[:, 32:, :64], own[:, 32:, 64:]], axis=1).reshape(1, D, 64)

    my_share = lax.axis_index(TP)
    first, second = route_expert[:, 0], route_expert[:, 1]
    group = first // 8
    experts = jnp.arange(64, dtype=jnp.int32)
    hot_first = first[:, None] == experts[None, :]
    hot_second = second[:, None] == experts[None, :]
    named = (hot_first | hot_second).astype(BF)
    row_at = jnp.arange(512, dtype=jnp.int32)
    before = (row_at[None, :] < row_at[:, None]).astype(BF)
    earlier = jnp.dot(before, named, preferred_element_type=F32)
    rank_first = jnp.sum(jnp.where(hot_first, earlier, 0.0), axis=1).astype(jnp.int32)
    rank_second = jnp.sum(jnp.where(hot_second, earlier, 0.0), axis=1).astype(jnp.int32)
    same_group = group[:, None] == experts[None, :] // 8
    rank_group = (jnp.sum(jnp.where(same_group, earlier, 0.0), axis=1) * 0.5).astype(jnp.int32)
    slot = group * 64 + rank_group

    def send_at(e, rank):
        return jnp.where(rank // 2 == my_share, ((e % 8) * 8 + e // 8) * 2 + rank % 2, -1)

    send_rows = jnp.arange(128, dtype=jnp.int32)[:, None]
    pick = (
        (send_at(first, rank_first)[None, :] == send_rows)
        | (send_at(second, rank_second)[None, :] == send_rows)
    ).astype(BF)
    chosen = jnp.dot(pick, tokens, preferred_element_type=F32)
    mean = jnp.mean(chosen * chosen, axis=1, keepdims=True)
    normed = (chosen * lax.rsqrt(mean + EPSILON)).astype(BF).reshape(64, 32, 128)

    gap = pair_logit[:, 0] - pair_logit[:, 1]
    weight_first = group_prob * jax.nn.sigmoid(gap)
    weight_second = group_prob * jax.nn.sigmoid(-gap)
    facts = jnp.stack(
        [
            ((first % 8) * 16 + rank_first).astype(F32),
            ((second % 8) * 16 + rank_second).astype(F32),
            weight_first,
            weight_second,
            jnp.zeros_like(gap),
            jnp.zeros_like(gap),
            jnp.zeros_like(gap),
            jnp.zeros_like(gap),
        ]
    ).astype(BF)
    to_slot = (slot[:, None] == row_at[None, :]).astype(BF)
    facts = jnp.dot(facts, to_slot, preferred_element_type=F32).astype(BF)
    facts = facts.reshape(8, 8, 64).transpose(1, 0, 2)
    got = trade_facts(facts, range(1, 7))
    sent, got = lax.optimization_barrier((normed, got))
    got.update(trade_facts(facts, (0, 7)))
    received = lax.all_to_all(
        sent, ("l", "y", "g"), split_axis=0, concat_axis=0, tiled=True
    )
    eight = jnp.arange(8, dtype=jnp.int32)
    from_group = ((lax.axis_index("g") - eight[:, None]) & 7 == eight[None, :]).astype(BF)
    facts = jnp.einsum("gk,kfr->fgr", from_group, jnp.stack([got[k] for k in range(8)]), preferred_element_type=F32)
    facts = facts.reshape(8, 512)
    code = facts[:2].astype(jnp.int32)
    source = row_at // 64
    at = (code // 16 * 8 + code % 16 // 2) * 16 + source[None, :] * 2 + code % 2
    slots = jnp.arange(1024, dtype=jnp.int32)[:, None]
    is_first, is_second = at[0][None, :] == slots, at[1][None, :] == slots
    mix = jnp.where(is_first, facts[2][None, :], jnp.where(is_second, facts[3][None, :], 0.0))
    mix = mix.astype(BF)
    outs = expert(received.reshape(128, D), gather_weights(own))
    back = lax.all_to_all(outs, IN_GROUP, split_axis=0, concat_axis=0, tiled=True)
    back = back.reshape(1024, 256)
    over_slots = (((0,), (0,)), ((), ()))
    mixed = lax.dot_general(mix, back, over_slots, preferred_element_type=F32).astype(BF)
    home = lax.all_to_all(
        mixed.reshape(8, 64, 256), "g", split_axis=0, concat_axis=0, tiled=True
    ).reshape(512, 256)
    home = pl.pallas_call(
        home_kernel, out_shape=jax.ShapeDtypeStruct((512, 256), BF), name="home"
    )(slot.reshape(1, 512), pltpu.with_memory_space_constraint(home, pltpu.VMEM))
    return new_gate, new_up, new_down, home


def solution(mesh):
    fine = Mesh(mesh.devices.reshape(8, 2, 4, 4, 2), ("g", "l", "y", "x", "c"))
    placed = (
        P(FS, None),
        P(FS),
        P(None, FS, TP),
        P(None, FS, TP),
        P(None, FS, TP),
        P(FS, None),
        P(FS),
        P(FS, None),
    )
    return jax.shard_map(
        local,
        mesh=fine,
        in_specs=placed,
        out_specs=(P(FS, None, TP), P(FS, None, TP), P(FS, None, TP), P(FS, TP)),
        check_vma=False,
    )
```

```python
import jax
import jax.numpy as jnp
from jax import lax
from jax.experimental import pallas as pl
from jax.experimental.pallas import tpu as pltpu
from jax.sharding import Mesh, PartitionSpec as P

D = 2048
EPSILON = 1e-06
FS = ("g", "l", "y")
TP = ("x", "c")
IN_GROUP = ("l", "y", "x", "c")
BF = jnp.bfloat16
F32 = jnp.float32


HELD = (0, 2, 6, 8)


def pack_kernel(gain_ref, gate_ref, up_ref, down_ref, out_ref):
    along = jnp.broadcast_to(gain_ref[...], (32, 32))
    diagonal = lax.broadcasted_iota(jnp.int32, (32, 32), 0) == lax.broadcasted_iota(
        jnp.int32, (32, 32), 1
    )
    gain = jnp.sum(jnp.where(diagonal, along, 0.0), axis=1, keepdims=True)[None]
    out_ref[:, :32, :64] = (gate_ref[...] * gain).astype(BF)
    out_ref[:, :32, 64:] = (up_ref[...] * gain).astype(BF)
    out_ref[:, 32:, :64] = down_ref[:, :16, :].astype(BF)
    out_ref[:, 32:, 64:] = down_ref[:, 16:, :].astype(BF)


def pack(norm_gain, w_gate, w_up, w_down):
    return pl.pallas_call(
        pack_kernel, out_shape=jax.ShapeDtypeStruct((64, 48, 128), BF), name="pack"
    )(norm_gain.reshape(1, 32), w_gate, w_up, w_down)


def home_kernel(slot_ref, back_ref, out_ref):
    row = lax.broadcasted_iota(jnp.int32, (512, 512), 0)
    at_slot = (row == slot_ref[...]).astype(F32).astype(BF)
    rows = lax.dot_general(
        at_slot, back_ref[...], (((0,), (0,)), ((), ())), preferred_element_type=F32
    ).astype(BF)
    lies = lax.broadcasted_iota(jnp.int32, (256, 256), 0)
    feature = lax.broadcasted_iota(jnp.int32, (256, 256), 1)
    lies_at = ((feature >> 4) & 1) * 128 + (feature >> 5) * 16 + (feature & 15)
    reorder = (lies == lies_at).astype(F32).astype(BF)
    out_ref[...] = jnp.dot(rows, reorder, preferred_element_type=F32).astype(BF)


def expert_kernel(x_ref, *refs):
    shards, out_ref, acc = refs[:8], refs[8], refs[9]
    x = x_ref[...]
    lane = lax.broadcasted_iota(jnp.int32, (128, 256), 1) % 128
    low = lane < 64
    pieces = []
    for k in range(4):
        pair = shards[2 * k : 2 * k + 2]
        both = jnp.concatenate([r[:, :32, :].reshape(-1, 128) for r in pair], axis=1)
        pre = jnp.dot(x, both, preferred_element_type=F32)
        other = jnp.concatenate(
            [pltpu.roll(pre[:, :128], 64, 1), pltpu.roll(pre[:, 128:], 64, 1)], axis=1
        )
        gate = jnp.where(low, pre, other)
        up = jnp.where(low, other, pre)
        hidden = gate / (1.0 + jnp.exp(-gate)) * up
        pieces.append(
            jnp.concatenate(
                [jnp.where(low, hidden, 0.0), jnp.where(low, 0.0, hidden)], axis=0
            ).astype(BF)
        )
    down = jnp.concatenate([r[:, 32:, :].reshape(-1, 128) for r in shards], axis=1)
    acc[...] = lax.dot_general(
        jnp.concatenate(pieces, axis=1),
        down,
        (((1,), (1,)), ((), ())),
        preferred_element_type=F32,
    )
    for j in range(8):
        for t in range(8):
            for h in range(2):
                out_ref[8 * j + t, :, 128 * h : 128 * (h + 1)] = acc[
                    128 * h + 16 * j : 128 * h + 16 * (j + 1), 128 * t : 128 * (t + 1)
                ].astype(BF)


def expert(rows, shards):
    operands = [rows, *shards]
    for i in HELD:
        operands[i] = pltpu.with_memory_space_constraint(operands[i], pltpu.VMEM)
    return pl.pallas_call(
        expert_kernel,
        out_shape=jax.ShapeDtypeStruct((64, 16, 256), BF),
        scratch_shapes=[pltpu.VMEM((256, 1024), F32)],
        name="expert",
    )(*operands)


def gather_weights(own):
    ring = [(i, (i + 1) % 4) for i in range(4)]
    around = [pair for i, j in ring for pair in ((2 * i, 2 * j), (2 * j + 1, 2 * i + 1))]
    back = [(j, i) for i, j in around]

    def pass_on(v, pairs):
        return lax.ppermute(v, TP, pairs)

    def swap(v):
        return lax.ppermute(v, "c", [(0, 1), (1, 0)])

    near, other = pass_on(own, around), pass_on(own, back)
    far = pass_on(near, around)
    own_c, near_c = swap(own), swap(near)
    other_c, far_c = swap(other), swap(far)
    return own, own_c, near, near_c, other, other_c, far, far_c


def trade_facts(facts, shifts):
    mine = lax.axis_index("g")
    got = {}
    for k in shifts:
        part = lax.dynamic_index_in_dim(facts, (mine + k) & 7, 0, keepdims=False)
        if k:
            part = lax.ppermute(part, "g", [(i, (i + k) % 8) for i in range(8)])
        got[k] = part
    return got


def local(tokens, norm_gain, w_gate, w_up, w_down, route_expert, group_prob, pair_logit):
    packed = pack(norm_gain, w_gate, w_up, w_down)
    own = lax.all_to_all(packed, FS, split_axis=0, concat_axis=0, tiled=True)
    new_gate = own[:, :32, :64].reshape(1, D, 64)
    new_up = own[:, :32, 64:].reshape(1, D, 64)
    new_down = jnp.concatenate([own[:, 32:, :64], own[:, 32:, 64:]], axis=1).reshape(1, D, 64)

    my_share = lax.axis_index(TP)
    first, second = route_expert[:, 0], route_expert[:, 1]
    group = first // 8
    experts = jnp.arange(64, dtype=jnp.int32)
    hot_first = first[:, None] == experts[None, :]
    hot_second = second[:, None] == experts[None, :]
    named = (hot_first | hot_second).astype(BF)
    row_at = jnp.arange(512, dtype=jnp.int32)
    before = (row_at[None, :] < row_at[:, None]).astype(BF)
    earlier = jnp.dot(before, named, preferred_element_type=F32)
    rank_first = jnp.sum(jnp.where(hot_first, earlier, 0.0), axis=1).astype(jnp.int32)
    rank_second = jnp.sum(jnp.where(hot_second, earlier, 0.0), axis=1).astype(jnp.int32)
    same_group = group[:, None] == experts[None, :] // 8
    rank_group = (jnp.sum(jnp.where(same_group, earlier, 0.0), axis=1) * 0.5).astype(jnp.int32)
    slot = group * 64 + rank_group

    def send_at(e, rank):
        return jnp.where(rank // 2 == my_share, ((e % 8) * 8 + e // 8) * 2 + rank % 2, -1)

    send_rows = jnp.arange(128, dtype=jnp.int32)[:, None]
    pick = (
        (send_at(first, rank_first)[None, :] == send_rows)
        | (send_at(second, rank_second)[None, :] == send_rows)
    ).astype(BF)
    chosen = jnp.dot(pick, tokens, preferred_element_type=F32)
    mean = jnp.mean(chosen * chosen, axis=1, keepdims=True)
    normed = (chosen * lax.rsqrt(mean + EPSILON)).astype(BF).reshape(64, 32, 128)

    gap = pair_logit[:, 0] - pair_logit[:, 1]
    weight_first = group_prob * jax.nn.sigmoid(gap)
    weight_second = group_prob * jax.nn.sigmoid(-gap)
    facts = jnp.stack(
        [
            ((first % 8) * 16 + rank_first).astype(F32),
            ((second % 8) * 16 + rank_second).astype(F32),
            weight_first,
            weight_second,
            jnp.zeros_like(gap),
            jnp.zeros_like(gap),
            jnp.zeros_like(gap),
            jnp.zeros_like(gap),
        ]
    ).astype(BF)
    to_slot = (slot[:, None] == row_at[None, :]).astype(BF)
    facts = jnp.dot(facts, to_slot, preferred_element_type=F32).astype(BF)
    facts = facts.reshape(8, 8, 64).transpose(1, 0, 2)
    got = trade_facts(facts, range(1, 7))
    sent, got = lax.optimization_barrier((normed, got))
    got.update(trade_facts(facts, (0, 7)))
    received = lax.all_to_all(
        sent, ("l", "y", "g"), split_axis=0, concat_axis=0, tiled=True
    )
    eight = jnp.arange(8, dtype=jnp.int32)
    from_group = ((lax.axis_index("g") - eight[:, None]) & 7 == eight[None, :]).astype(BF)
    facts = jnp.einsum("gk,kfr->fgr", from_group, jnp.stack([got[k] for k in range(8)]), preferred_element_type=F32)
    facts = facts.reshape(8, 512)
    code = facts[:2].astype(jnp.int32)
    source = row_at // 64
    at = (code // 16 * 8 + code % 16 // 2) * 16 + source[None, :] * 2 + code % 2
    slots = jnp.arange(1024, dtype=jnp.int32)[:, None]
    is_first, is_second = at[0][None, :] == slots, at[1][None, :] == slots
    mix = jnp.where(is_first, facts[2][None, :], jnp.where(is_second, facts[3][None, :], 0.0))
    mix = mix.astype(BF)
    outs = expert(received.reshape(128, D), gather_weights(own))
    back = lax.all_to_all(outs, IN_GROUP, split_axis=0, concat_axis=0, tiled=True)
    back = back.reshape(1024, 256)
    over_slots = (((0,), (0,)), ((), ()))
    mixed = lax.dot_general(mix, back, over_slots, preferred_element_type=F32).astype(BF)
    home = lax.all_to_all(
        mixed.reshape(8, 64, 256), "g", split_axis=0, concat_axis=0, tiled=True
    ).reshape(512, 256)
    home = pl.pallas_call(
        home_kernel, out_shape=jax.ShapeDtypeStruct((512, 256), BF), name="home"
    )(slot.reshape(1, 512), pltpu.with_memory_space_constraint(home, pltpu.VMEM))
    return new_gate, new_up, new_down, home


def solution(mesh):
    fine = Mesh(mesh.devices.reshape(8, 2, 4, 4, 2), ("g", "l", "y", "x", "c"))
    placed = (
        P(FS, None),
        P(FS),
        P(None, FS, TP),
        P(None, FS, TP),
        P(None, FS, TP),
        P(FS, None),
        P(FS),
        P(FS, None),
    )
    return jax.shard_map(
        local,
        mesh=fine,
        in_specs=placed,
        out_specs=(P(FS, None, TP), P(FS, None, TP), P(FS, None, TP), P(FS, TP)),
        check_vma=False,
    )
```
